32 devices in a mesh: fs: 8 (over z, y), tp: 4 (over x, core).
Axes of the slice: x: 2, y: 2, z: 4, core: 2. Of those that a mesh axis runs over, the one named last changes fastest.
Arguments:
- tokens: bfloat16 [1280, 2048], P('fs', 'tp'), may hold values from -6 to 6
- mix_gain: float32 [2048], replicated, may hold values from 0.1 to 1.9
- in_x_w: bfloat16 [2048, 1024], P('fs', 'tp'), may hold values from -0.125 to 0.125
- in_gate_w: bfloat16 [2048, 1024], P('fs', 'tp'), may hold values from -0.125 to 0.125
- conv_taps: float32 [4, 1024], P(None, 'tp'), may hold values from -3 to 3
- gate_x_blocks: bfloat16 [8, 128, 128], P('tp'), may hold values from -0.5 to 0.5
- gate_a_blocks: bfloat16 [8, 128, 128], P('tp'), may hold values from -0.5 to 0.5
- forget_rate: float32 [1024], P('tp'), may hold values from 0.002 to 0.08
- out_w: bfloat16 [1024, 2048], P('tp', 'fs'), may hold values from -0.1875 to 0.1875
- ffn_gain: float32 [2048], replicated, may hold values from 0.1 to 1.9
- ffn_gate_w: bfloat16 [2048, 2816], P('fs', 'tp'), may hold values from -0.125 to 0.125
- ffn_up_w: bfloat16 [2048, 2816], P('fs', 'tp'), may hold values from -0.125 to 0.125
- ffn_down_w: bfloat16 [2816, 2048], P('tp', 'fs'), may hold values from -0.109375 to 0.109375
Outputs:
- layer_out: bfloat16 [1280, 2048], P('fs', 'tp')
The draws below stay inside these ranges and needn't reach their ends.
All inputs are finite; a program needn't handle non-finite values.
Results may differ from the reference program's by a relative error of at most 0.015.
Values may be sent and summed in bfloat16 or wider, within the bound.
No kernel may reach another device: no remote copies, remote signals or barrier semaphores. Data moves between devices by JAX's collectives and lax.ppermute only.
A program may use at most 64 MiB of HBM per device.

```python
import math
import jax
import jax.numpy as jnp
from jax import lax

D = 2048
BLOCK_DIM = 128
RG_BLOCKS = 8
RG = 1024
FF = 2816
TAPS = 4
TOK_DEV = 160
TOKENS = 1280
N_FS = 8
N_TP = 4


def steps_of(stream_key, shape, pieces, least, top_value):
    loudness, own = 1.0, jax.random.fold_in(stream_key, 6)
    for position, blocks in pieces:
        steps = jnp.exp(jax.random.uniform(jax.random.fold_in(own, position), (blocks,), jnp.float32, least / len(pieces), top_value / len(pieces)))
        loudness = loudness * jnp.repeat(steps, shape[position] // blocks).reshape([-1 if axis == position else 1 for axis in range(len(shape))])
    return loudness


def scatter_about(stream_key, dims, spread, limit, pieces=(), dtype=jnp.bfloat16):
    result = spread * jax.random.normal(stream_key, dims, jnp.float32)
    if pieces:
        result = result * steps_of(stream_key, dims, pieces, -0.22, 0.18)
    return jnp.clip(result, -limit, limit).astype(dtype)


def setup_inputs(seed: int = 0) -> dict:
    streams_of = jax.random.split(jax.random.key(seed), 14)
    return {
        "tokens": scatter_about(streams_of[0], (TOKENS, D), 1.0, 6.0, ((0, 8), (1, 4))),
        "mix_gain": jnp.clip(1.0 + 0.18 * jax.random.normal(streams_of[1], (D,), jnp.float32), 0.1, 1.9),
        "in_x_w": scatter_about(streams_of[2], (D, RG), D ** -0.5, 0.125, ((0, 8), (1, 4))),
        "in_gate_w": scatter_about(streams_of[3], (D, RG), D ** -0.5, 0.125, ((0, 8), (1, 4))),
        "conv_taps": scatter_about(streams_of[4], (TAPS, RG), TAPS ** -0.5, 3.0, ((1, 4),), jnp.float32),
        "gate_x_blocks": scatter_about(streams_of[5], (RG_BLOCKS, BLOCK_DIM, BLOCK_DIM), BLOCK_DIM ** -0.5, 0.5, ((0, 4),)),
        "gate_a_blocks": scatter_about(streams_of[6], (RG_BLOCKS, BLOCK_DIM, BLOCK_DIM), BLOCK_DIM ** -0.5, 0.5, ((0, 4),)),
        "forget_rate": jnp.clip(jnp.exp(math.log(0.08) - 3.6888794 * jax.random.uniform(streams_of[7], (RG,), jnp.float32) ** steps_of(streams_of[7], (RG,), ((0, 4),), -0.2, 0.2)), 0.002, 0.08),
        "out_w": scatter_about(streams_of[8], (RG, D), RG ** -0.5, 0.1875, ((0, 4), (1, 8))),
        "ffn_gain": jnp.clip(1.0 + 0.18 * jax.random.normal(streams_of[9], (D,), jnp.float32), 0.1, 1.9),
        "ffn_gate_w": scatter_about(streams_of[10], (D, FF), D ** -0.5, 0.125, ((0, 8), (1, 4))),
        "ffn_up_w": scatter_about(streams_of[11], (D, FF), D ** -0.5, 0.125, ((0, 8), (1, 4))),
        "ffn_down_w": scatter_about(streams_of[12], (FF, D), FF ** -0.5, 0.109375, ((0, 4), (1, 8))),
    }


epsilon = 1e-06
gate_power = 8.0

def rms_norm(values, gain):
    wide = values.astype(jnp.float32)
    mean_square = lax.optimization_barrier(jnp.mean(wide * wide, axis=-1, keepdims=True))
    return (wide * lax.rsqrt(mean_square + epsilon) * gain).astype(jnp.bfloat16)

def grouped_sum(acts, weight):
    group_width = acts.shape[1] // N_TP
    total = jnp.zeros((acts.shape[0], weight.shape[1]), jnp.float32)
    for index in range(N_TP):
        part = jnp.dot(acts[:, index * group_width:(index + 1) * group_width], weight[index * group_width:(index + 1) * group_width], preferred_element_type=jnp.float32)
        part = lax.optimization_barrier(part.astype(jnp.bfloat16))
        total = total + part.astype(jnp.float32)
    return total

def combine(earlier, later):
    return (earlier[0] * later[0], later[0] * earlier[1] + later[1])

def reference(tokens, mix_gain, in_x_w, in_gate_w, conv_taps, gate_x_blocks, gate_a_blocks, forget_rate, out_w, ffn_gain, ffn_gate_w, ffn_up_w, ffn_down_w):
    normed = rms_norm(tokens, mix_gain)
    branch_in = jnp.dot(normed, in_x_w, preferred_element_type=jnp.float32).reshape(N_FS, TOK_DEV, RG)
    branch_gate = jnp.dot(normed, in_gate_w, preferred_element_type=jnp.float32).reshape(N_FS, TOK_DEV, RG)
    padded = jnp.pad(branch_in, ((0, 0), (TAPS - 1, 0), (0, 0)))
    conv_sum = padded[:, 0:TOK_DEV] * conv_taps[0]
    for index in range(1, TAPS):
        conv_sum = conv_sum + padded[:, index:index + TOK_DEV] * conv_taps[index]
    conv_out = conv_sum.astype(jnp.bfloat16)
    grouped = conv_out.reshape(N_FS, TOK_DEV, RG_BLOCKS, BLOCK_DIM).astype(jnp.float32)
    gate_x = jax.nn.sigmoid(jnp.einsum('stbi,bij->stbj', grouped, gate_x_blocks.astype(jnp.float32)).reshape(N_FS, TOK_DEV, RG))
    gate_a = jax.nn.sigmoid(jnp.einsum('stbi,bij->stbj', grouped, gate_a_blocks.astype(jnp.float32)).reshape(N_FS, TOK_DEV, RG))
    log_decay = -gate_power * gate_a * forget_rate
    decay = jnp.exp(log_decay)
    scale = jnp.sqrt(-jnp.expm1(2.0 * log_decay))
    first = (jnp.arange(TOK_DEV) == 0)[None, :, None]
    scale = jnp.where(first, 1.0, scale)
    driven = conv_out.astype(jnp.float32) * gate_x * scale
    _, state = lax.associative_scan(combine, (decay, driven), axis=1)
    mixer_out = (state * jax.nn.gelu(branch_gate)).reshape(TOKENS, RG).astype(jnp.bfloat16)
    after_mix = (tokens.astype(jnp.float32) + grouped_sum(mixer_out, out_w)).astype(jnp.bfloat16)
    normed_ffn = rms_norm(after_mix, ffn_gain)
    gate_val = jnp.dot(normed_ffn, ffn_gate_w, preferred_element_type=jnp.float32)
    up_val = jnp.dot(normed_ffn, ffn_up_w, preferred_element_type=jnp.float32)
    hidden = (jax.nn.silu(gate_val) * up_val).astype(jnp.bfloat16)
    return (after_mix.astype(jnp.float32) + grouped_sum(hidden, ffn_down_w)).astype(jnp.bfloat16)
```

```python
import jax
import jax.numpy as jnp
from jax import lax
from jax.sharding import PartitionSpec as P

epsilon = 1e-06
gate_power = 8.0


def combine(earlier, later):
    return (earlier[0] * later[0], later[0] * earlier[1] + later[1])


def dot(left, right):
    return jnp.dot(left, right, preferred_element_type=jnp.float32)


def layer(n_fs, n_tp):
    low = min(n_fs, 8)
    highs = [bit for bit in range(3, 12) if (1 << bit) < n_fs]
    per_tp = n_fs // n_tp

    def fs_swap(values, mask):
        return lax.ppermute(values, "fs", [(j, j ^ mask) for j in range(n_fs)])

    def swap(values, fs_mask, tp_mask):
        pairs = [
            (a * n_tp + b, (a ^ fs_mask) * n_tp + (b ^ tp_mask))
            for a in range(n_fs)
            for b in range(n_tp)
        ]
        return lax.ppermute(values, ("fs", "tp"), pairs)

    def on_device(
        tokens,
        mix_gain,
        in_x_w,
        in_gate_w,
        conv_taps,
        gate_x_blocks,
        gate_a_blocks,
        forget_rate,
        out_w,
        ffn_gain,
        ffn_gate_w,
        ffn_up_w,
        ffn_down_w,
    ):
        fs = lax.axis_index("fs")
        tp = lax.axis_index("tp")
        blocks = gate_x_blocks.shape[0]
        mate = 2 if blocks % 2 == 0 and n_fs >= 4 else 0
        group = 2 if mate else 1
        side = (fs // mate) % 2 if mate else 0
        length, width = tokens.shape

        def half(values, which, axis):
            if not mate:
                return values
            size = values.shape[axis] // 2
            return lax.dynamic_slice_in_dim(values, which * size, size, axis)

        def gather(mine, other):
            mine = mine[None]
            other = other[None]
            for bit in highs:
                mine = jnp.concatenate([mine, fs_swap(mine, 1 << bit)])
                other = jnp.concatenate([other, fs_swap(other, 1 << bit)]) if mate else mine
            got = {0: mine}
            for step in range(2, low, 2):
                got[step] = fs_swap(other if step & mate else mine, step)
            for step in range(0, low, 2):
                got[step ^ 1] = fs_swap(got[step], 1)
            return got

        def members(step):
            return fs ^ step ^ (jnp.arange(1 << len(highs)) << 3)

        def whole_rows(own):
            parts = []
            for step in range(0, n_tp, 2):
                for far in range(group):
                    moved = own if step == 0 and far == 0 else swap(own, mate * far, step)
                    parts.append(moved)
            near = jnp.stack(parts).reshape(n_tp // 2, group * length, width)
            across = lax.ppermute(near, "tp", [(j, j ^ 1) for j in range(n_tp)])
            return jnp.stack([near, across], axis=1).reshape(n_tp, group * length, width)

        def rms_norm(rows, gain):
            wide = rows.astype(jnp.float32)
            mean_square = jnp.sum(wide * wide, axis=(0, 2), keepdims=True) / (n_tp * width)
            gains = jnp.take(gain.reshape(n_tp, 1, width), tp ^ jnp.arange(n_tp), axis=0)
            return (wide * lax.rsqrt(mean_square + epsilon) * gains).astype(jnp.bfloat16)

        def project(rows, weights):
            depth = n_tp * width // n_fs
            total = None
            if highs:
                order = tp ^ jnp.arange(n_tp)
                rows = jnp.take(rows, order, axis=0).reshape(n_tp, rows.shape[1], per_tp, depth)
                rows = rows.transpose(1, 0, 2, 3).reshape(rows.shape[1], n_fs, depth)
            for step, block in weights.items():
                if highs:
                    left = jnp.take(rows, members(step), axis=1)
                    left = left.reshape(rows.shape[0], -1)
                else:
                    source = fs ^ step
                    start = (tp ^ (source // per_tp), 0, (source % per_tp) * depth)
                    left = lax.dynamic_slice(rows, start, (1, rows.shape[1], depth))[0]
                part = dot(left, block.reshape(-1, block.shape[-1]))
                total = part if total is None else total + part
            return total

        def project_out(acts, weights):
            columns = n_tp * width // n_fs
            parts = []
            order = []
            for step, block in weights.items():
                for index in range(block.shape[0]):
                    parts.append(dot(acts, block[index]).astype(jnp.bfloat16))
                    order.append(step ^ (index << 3))
            place = [order.index(i) for i in range(n_fs)]
            stacked = jnp.stack([parts[i] for i in place])
            stacked = stacked.reshape(n_fs, group, length, columns)

            def towards(step):
                target = fs ^ ((tp ^ step) * per_tp + jnp.arange(per_tp))
                if per_tp == 1:
                    return lax.dynamic_index_in_dim(stacked, target[0], 0, False)
                picked = [
                    lax.dynamic_index_in_dim(stacked, target[i], 0, False) for i in range(per_tp)
                ]
                return jnp.concatenate(picked, axis=-1)

            across = jnp.stack([towards(step ^ 1) for step in range(0, n_tp, 2)])
            across = lax.ppermute(across, "tp", [(j, j ^ 1) for j in range(n_tp)])
            total = None
            for at, step in enumerate(range(0, n_tp, 2)):
                near = towards(step).astype(jnp.float32) + across[at].astype(jnp.float32)
                for far in range(group):
                    if step == 0 and far == 0:
                        part = near[0]
                    else:
                        sent = near[far].astype(jnp.bfloat16)
                        part = swap(sent, mate * far, step).astype(jnp.float32)
                    total = part if total is None else total + part
            return total

        def in_halves(which):
            return jnp.concatenate([half(in_x_w, which, 1), half(in_gate_w, which, 1)], axis=1)

        def up_halves(which):
            return jnp.concatenate([half(ffn_gate_w, which, 1), half(ffn_up_w, which, 1)], axis=1)

        rows = whole_rows(tokens)
        in_w = gather(in_halves(side), in_halves(1 - side))
        out_blocks = gather(half(out_w, side, 0), half(out_w, 1 - side, 0))
        up_w = gather(up_halves(side), up_halves(1 - side))
        down_w = gather(half(ffn_down_w, side, 0), half(ffn_down_w, 1 - side, 0))

        normed = rms_norm(rows, mix_gain)
        branches = project(normed, in_w)
        chans = branches.shape[1] // 2
        branch_in = branches[:, :chans].reshape(group, length, chans)
        branch_gate = branches[:, chans:].reshape(group, length, chans)
        taps = half(conv_taps, side, 1)
        tap_count = taps.shape[0]
        padded = jnp.pad(branch_in, ((0, 0), (tap_count - 1, 0), (0, 0)))
        conv_sum = padded[:, 0:length] * taps[0]
        for index in range(1, tap_count):
            conv_sum = conv_sum + padded[:, index : index + length] * taps[index]
        conv_out = conv_sum.astype(jnp.bfloat16)
        x_blocks = half(gate_x_blocks, side, 0)
        a_blocks = half(gate_a_blocks, side, 0)
        size = x_blocks.shape[1]

        def gate(maps):
            pieces = [
                dot(conv_out[:, :, i * size : (i + 1) * size].reshape(group * length, size), maps[i])
                for i in range(maps.shape[0])
            ]
            return jax.nn.sigmoid(jnp.concatenate(pieces, axis=1).reshape(group, length, chans))

        gate_x = gate(x_blocks)
        gate_a = gate(a_blocks)
        log_decay = -gate_power * gate_a * half(forget_rate, side, 0)
        decay = jnp.exp(log_decay)
        scale = jnp.sqrt(-jnp.expm1(2.0 * log_decay))
        scale = jnp.where((jnp.arange(length) == 0)[None, :, None], 1.0, scale)
        driven = conv_out.astype(jnp.float32) * gate_x * scale
        _, state = lax.associative_scan(combine, (decay, driven), axis=1)
        mixer_out = (state * jax.nn.gelu(branch_gate)).astype(jnp.bfloat16)
        mixer_out = mixer_out.reshape(group * length, chans)
        after_mix = (tokens.astype(jnp.float32) + project_out(mixer_out, out_blocks)).astype(jnp.bfloat16)
        normed_ffn = rms_norm(whole_rows(after_mix), ffn_gain)
        gates = project(normed_ffn, up_w)
        units = gates.shape[1] // 2
        hidden = (jax.nn.silu(gates[:, :units]) * gates[:, units:]).astype(jnp.bfloat16)
        return (after_mix.astype(jnp.float32) + project_out(hidden, down_w)).astype(jnp.bfloat16)

    return on_device


def solution(mesh):
    placed = (
        P("fs", "tp"),
        P(),
        P("fs", "tp"),
        P("fs", "tp"),
        P(None, "tp"),
        P("tp", None, None),
        P("tp", None, None),
        P("tp"),
        P("tp", "fs"),
        P(),
        P("fs", "tp"),
        P("fs", "tp"),
        P("tp", "fs"),
    )
    return jax.shard_map(
        layer(mesh.shape["fs"], mesh.shape["tp"]),
        mesh=mesh,
        in_specs=placed,
        out_specs=P("fs", "tp"),
        check_vma=False,
    )
```

```python
import functools

import jax
import jax.numpy as jnp
from jax import lax
from jax.experimental import pallas as pl
from jax.experimental.pallas import tpu as pltpu
from jax.sharding import PartitionSpec as P

epsilon = 1e-06
gate_power = 8.0


def dot(left, right):
    return jnp.dot(left, right, preferred_element_type=jnp.float32)


def rms_norm(values, gain):
    wide = values.astype(jnp.float32)
    mean_square = jnp.mean(wide * wide, axis=-1, keepdims=True)
    return (wide * lax.rsqrt(mean_square + epsilon) * gain).astype(jnp.bfloat16)


def full_rows(shard):
    return lax.all_gather(shard, "tp", axis=1, tiled=True)


def project_out(acts, weight):
    partial_terms = dot(acts, lax.all_gather(weight, "fs", axis=1, tiled=True))
    return lax.psum_scatter(
        partial_terms.astype(jnp.bfloat16), "tp", scatter_dimension=1, tiled=True
    ).astype(jnp.float32)


def combine(earlier, later):
    return (earlier[0] * later[0], later[0] * earlier[1] + later[1])


def gathered_layer(
    tokens,
    mix_gain,
    in_x_w,
    in_gate_w,
    conv_taps,
    gate_x_blocks,
    gate_a_blocks,
    forget_rate,
    out_w,
    ffn_gain,
    ffn_gate_w,
    ffn_up_w,
    ffn_down_w,
):
    normed = rms_norm(full_rows(tokens), mix_gain)
    length = normed.shape[0]
    chan_width = in_x_w.shape[1]
    branch_in = dot(normed, lax.all_gather(in_x_w, "fs", axis=0, tiled=True))
    branch_gate = dot(normed, lax.all_gather(in_gate_w, "fs", axis=0, tiled=True))
    tap_count = conv_taps.shape[0]
    padded = jnp.pad(branch_in, ((tap_count - 1, 0), (0, 0)))
    conv_sum = padded[0:length] * conv_taps[0]
    for index in range(1, tap_count):
        conv_sum = conv_sum + padded[index : index + length] * conv_taps[index]
    conv_out = conv_sum.astype(jnp.bfloat16)
    blocks, block_dim = gate_x_blocks.shape[:2]
    grouped = conv_out.reshape(length, blocks, block_dim)

    def gate(maps):
        mapped = jnp.einsum("tbi,bij->tbj", grouped, maps, preferred_element_type=jnp.float32)
        return jax.nn.sigmoid(mapped.reshape(length, chan_width))

    log_decay = -gate_power * gate(gate_a_blocks) * forget_rate
    scale = jnp.sqrt(-jnp.expm1(2.0 * log_decay))
    scale = jnp.where((jnp.arange(length) == 0)[:, None], 1.0, scale)
    driven = conv_out.astype(jnp.float32) * gate(gate_x_blocks) * scale
    _, state = lax.associative_scan(combine, (jnp.exp(log_decay), driven), axis=0)
    mixer_out = (state * jax.nn.gelu(branch_gate)).astype(jnp.bfloat16)
    after_mix = (tokens.astype(jnp.float32) + project_out(mixer_out, out_w)).astype(jnp.bfloat16)
    normed_ffn = rms_norm(full_rows(after_mix), ffn_gain)
    gate_val = dot(normed_ffn, lax.all_gather(ffn_gate_w, "fs", axis=0, tiled=True))
    up_val = dot(normed_ffn, lax.all_gather(ffn_up_w, "fs", axis=0, tiled=True))
    hidden = (jax.nn.silu(gate_val) * up_val).astype(jnp.bfloat16)
    return (after_mix.astype(jnp.float32) + project_out(hidden, ffn_down_w)).astype(jnp.bfloat16)


MATE = 2
GROUP = 2
KERNEL_BYTES = 16 << 20


def side_of(fs):
    return lax.rem(lax.div(fs, MATE), 2)


def turn_of(tp):
    return (tp & 1) * 4 + ((tp >> 1) ^ (tp & 1))


def block_of(fs, entry, count):
    back = ((fs >> 1) - entry // 2) & (count // 2 - 1)
    return back * 2 + ((fs & 1) ^ (entry & 1))


def at(index, size):
    return pl.ds(pl.multiple_of(index * size, size), size)


def call(kernel, outs, args, scratch=(), space=pltpu.VMEM):
    spec = pl.BlockSpec(memory_space=pltpu.VMEM)
    return pl.pallas_call(
        kernel,
        out_shape=outs,
        in_specs=[spec] * len(args),
        out_specs=jax.tree.map(lambda _: spec, outs),
        scratch_shapes=list(scratch),
        compiler_params=pltpu.CompilerParams(vmem_limit_bytes=KERNEL_BYTES),
    )(*[pltpu.with_memory_space_constraint(arg, space) for arg in args])


def split_in_kernel(x_ref, gate_ref, mine_ref, other_ref):
    side = side_of(lax.axis_index("fs"))
    half = x_ref.shape[1] // 2
    for out, which in ((mine_ref, side), (other_ref, 1 - side)):
        out[:, :half] = x_ref[:, at(which, half)]
        out[:, half:] = gate_ref[:, at(which, half)]


def split_ffn_kernel(gate_ref, up_ref, down_ref, *results):
    side = side_of(lax.axis_index("fs"))
    half = gate_ref.shape[0] // 2
    for turn, which in enumerate((side, 1 - side)):
        up_part, down_part = results[2 * turn : 2 * turn + 2]
        up_part[:half] = gate_ref[at(which, half), :]
        up_part[half:] = up_ref[at(which, half), :]
        down_part[...] = down_ref[at(which, half), :]


def normalize(tp, row_refs, gain_ref, normed_ref):
    length, width = row_refs[0].shape
    slots = len(row_refs) // 2
    features = slots // GROUP * 2 * width
    for far in range(GROUP):
        pieces = []
        squares = 0.0
        for pair in range(slots // GROUP):
            for odd in range(2):
                wide = row_refs[odd * slots + pair * GROUP + far][...].astype(jnp.float32)
                squares = squares + jnp.sum(wide * wide, axis=1, keepdims=True)
                pieces.append((2 * pair + odd, wide))
        norm = lax.rsqrt(squares / features + epsilon)
        for step, wide in pieces:
            lanes = at(tp ^ step, width)
            scaled = wide * norm * gain_ref[:, lanes]
            normed_ref[far * length : (far + 1) * length, lanes] = scaled.astype(jnp.bfloat16)


def minus_expm1(value):
    series = 1.0 / 5040.0
    for factor in (720.0, 120.0, 24.0, 6.0, 2.0, 1.0):
        series = series * value + 1.0 / factor
    return jnp.where(value > -0.25, -value * series, 1.0 - jnp.exp(value))


def mixer_kernel(
    pieces, gain_ref, taps_ref, x_maps_ref, a_maps_ref, rate_ref, *rest
):
    row_refs, weights = rest[:pieces], rest[pieces:-3]
    out_ref, normed_ref, padded_ref = rest[-3:]
    fs = lax.axis_index("fs")
    tp = lax.axis_index("tp")
    side = side_of(fs)
    length = row_refs[0].shape[0]
    normalize(tp, row_refs, gain_ref, normed_ref)
    depth = weights[0].shape[0]
    branches = dot(normed_ref[:, at(fs, depth)], weights[0][...])
    for step in range(1, len(weights)):
        lanes = at(block_of(fs, step, len(weights)), depth)
        branches = branches + dot(normed_ref[:, lanes], weights[step][...])
    chans = out_ref.shape[1]
    tap_count = taps_ref.shape[0]
    taps = taps_ref[:, at(side, chans)]
    rate = rate_ref[:, at(side, chans)]
    maps = x_maps_ref.shape[0] // 2
    size = x_maps_ref.shape[1]
    lead = padded_ref.shape[0] - length
    row = lax.broadcasted_iota(jnp.int32, (length, chans), 0)
    padded_ref[:lead] = jnp.zeros((lead, chans), jnp.float32)
    for far in range(GROUP):
        rows = slice(far * length, (far + 1) * length)
        padded_ref[lead:] = branches[rows, :chans]
        first = lead - tap_count + 1
        conv_sum = padded_ref[first : first + length] * taps[0:1]
        for index in range(1, tap_count):
            start = first + index
            conv_sum = conv_sum + padded_ref[start : start + length] * taps[index : index + 1]
        conv_out = conv_sum.astype(jnp.bfloat16)

        def gate(maps_ref):
            parts = [
                dot(conv_out[:, i * size : (i + 1) * size], maps_ref[side * maps + i])
                for i in range(maps)
            ]
            return jax.nn.sigmoid(jnp.concatenate(parts, axis=1) if maps > 1 else parts[0])

        log_decay = -gate_power * gate(a_maps_ref) * rate
        decay = jnp.exp(log_decay)
        scale = jnp.where(row == 0, 1.0, jnp.sqrt(minus_expm1(2.0 * log_decay)))
        state = conv_out.astype(jnp.float32) * gate(x_maps_ref) * scale
        reach = 1
        while reach < length:
            begun = row >= reach
            state = state + decay * jnp.where(begun, pltpu.roll(state, reach, 0), 0.0)
            decay = decay * jnp.where(begun, pltpu.roll(decay, reach, 0), 1.0)
            reach *= 2
        out_ref[rows, :] = (state * jax.nn.gelu(branches[rows, chans:])).astype(jnp.bfloat16)


def halves_of(ref, far):
    length = ref.shape[0] // GROUP
    return [ref[((slot ^ far) * length) : ((slot ^ far) + 1) * length] for slot in range(GROUP)]


def mix_project_kernel(pieces, *refs):
    mixed, rows, weights = refs[:pieces], refs[pieces : 2 * pieces], refs[2 * pieces : -1]
    out_ref = refs[-1]
    fs = lax.axis_index("fs")
    tp = lax.axis_index("tp")
    side = side_of(fs)
    slots = pieces // 2
    length, width = rows[0].shape
    chans = mixed[0].shape[1]
    columns = weights[0].shape[1]
    block = fs ^ turn_of(tp)
    per_tp = width // columns
    owner = tp ^ lax.div(block, per_tp)
    lanes = at(lax.rem(block, per_tp), columns)
    totals = []
    for slot in range(GROUP):
        base = rows[slot][:, lanes]
        for step in range(1, slots // GROUP * 2):
            source = rows[(step & 1) * slots + step // 2 * GROUP + slot]
            base = jnp.where(owner == step, source[:, lanes], base)
        totals.append(base.astype(jnp.float32))
    for far in range(GROUP):
        which = at(side ^ far, chans)
        for step in range(slots // GROUP * 2):
            source = mixed[(step & 1) * slots + step // 2 * GROUP + far]
            part = dot(source[...], weights[step][which, :])
            for slot in range(GROUP):
                start = (slot ^ far) * length
                totals[slot] = totals[slot] + part[start : start + length]
    for slot in range(GROUP):
        out_ref[slot * length : (slot + 1) * length] = totals[slot].astype(jnp.bfloat16)


def hidden_kernel(pieces, gain_ref, *rest):
    row_refs, weights = rest[:pieces], rest[pieces:-4]
    out_ref, own_ref, normed_ref, whole_ref = rest[-4:]
    fs = lax.axis_index("fs")
    tp = lax.axis_index("tp")
    slots = pieces // 2
    length, width = own_ref.shape
    columns = row_refs[0].shape[1]
    features = columns * pieces
    squares = [0.0] * GROUP
    found = []
    for odd in range(2):
        for pair in range(slots // GROUP):
            for far in range(GROUP):
                source = row_refs[odd * slots + pair * GROUP + far]
                block = fs ^ (MATE * far) ^ turn_of(tp ^ (2 * pair + odd))
                halves = halves_of(source, far)
                whole_ref[:, at(block, columns)] = halves[0]
                wide = [half.astype(jnp.float32) for half in halves]
                for slot in range(GROUP):
                    row_sum = jnp.sum(wide[slot] * wide[slot], axis=1, keepdims=True)
                    squares[slot] = squares[slot] + row_sum
                found.append((at(block, columns), wide))
    norms = [lax.rsqrt(total / features + epsilon) for total in squares]
    for lanes, wide in found:
        for slot in range(GROUP):
            scaled = wide[slot] * norms[slot] * gain_ref[:, lanes]
            normed_ref[slot * length : (slot + 1) * length, lanes] = scaled.astype(jnp.bfloat16)
    own_ref[...] = whole_ref[:, at(tp, width)]
    units = out_ref.shape[1]
    depth = weights[0].shape[1]

    def project(first):
        total = None
        for step, weight in enumerate(weights):
            part = lax.dot_general(
                normed_ref[:, at(block_of(fs, step, len(weights)), depth)],
                weight[first : first + units, :],
                (((1,), (1,)), ((), ())),
                preferred_element_type=jnp.float32,
            )
            total = part if total is None else total + part
        return total

    out_ref[...] = (jax.nn.silu(project(0)) * project(units)).astype(jnp.bfloat16)


def project_out_kernel(acts_ref, *rest):
    *weights, send_ref, keep_ref, whole_ref = rest
    fs = lax.axis_index("fs")
    tp = lax.axis_index("tp")
    slots, length, width = keep_ref.shape
    columns = weights[0].shape[1]
    for step, weight in enumerate(weights):
        whole_ref[:, at(block_of(fs, step, len(weights)), columns)] = weight[...]
    for step in range(slots // GROUP * 2):
        part = dot(acts_ref[...], whole_ref[:, at(tp ^ step, width)]).astype(jnp.bfloat16)
        target = send_ref if step % 2 else keep_ref
        for far in range(GROUP):
            target[step // 2 * GROUP + far] = part[far * length : (far + 1) * length]


def join_kernel(keep_ref, got_ref, own_ref, *sent):
    own_ref[...] = keep_ref[0].astype(jnp.float32) + got_ref[0].astype(jnp.float32)
    for slot, out in enumerate(sent, 1):
        total = keep_ref[slot].astype(jnp.float32) + got_ref[slot].astype(jnp.float32)
        out[...] = total.astype(jnp.bfloat16)


def finish_kernel(base_ref, own_ref, *rest):
    *parts, out_ref = rest
    total = own_ref[...]
    for part in parts:
        total = total + part[...].astype(jnp.float32)
    out_ref[...] = (base_ref[...].astype(jnp.float32) + total).astype(jnp.bfloat16)


def paired_layer(n_fs, n_tp):
    def fs_swap(values, mask):
        return lax.ppermute(values, "fs", [(j, j ^ mask) for j in range(n_fs)])

    def core_swap(values):
        return lax.ppermute(values, "tp", [(j, j ^ 1) for j in range(n_tp)])

    def swap(values, fs_mask, tp_mask):
        pairs = [
            (a * n_tp + b, (a ^ fs_mask) * n_tp + (b ^ tp_mask))
            for a in range(n_fs)
            for b in range(n_tp)
        ]
        return lax.ppermute(values, ("fs", "tp"), pairs)

    def gather(mine, other):
        got = []
        for back in range(n_fs // 2):
            piece = mine
            if back:
                pairs = [(a, (a + 2 * back) % n_fs) for a in range(n_fs)]
                piece = lax.ppermute(other if back % 2 else mine, "fs", pairs)
            got += [piece, fs_swap(piece, 1)]
        return got

    def columns_of(shard):
        blocks = []
        for step in range(n_tp):
            pairs = [
                ((a ^ turn_of(b)) * n_tp + (b ^ step), a * n_tp + b)
                for a in range(n_fs)
                for b in range(n_tp)
            ]
            blocks.append(lax.ppermute(shard, ("fs", "tp"), pairs))
        return blocks

    def whole_rows(own):
        near = [own, swap(own, MATE, 0)]
        for step in range(2, n_tp, 2):
            near += [swap(piece, 0, step) for piece in near[:GROUP]]
        across = [core_swap(piece) for piece in near]
        return near + across

    def on_device(
        tokens,
        mix_gain,
        in_x_w,
        in_gate_w,
        conv_taps,
        gate_x_blocks,
        gate_a_blocks,
        forget_rate,
        out_w,
        ffn_gain,
        ffn_gate_w,
        ffn_up_w,
        ffn_down_w,
    ):
        length, width = tokens.shape
        features = n_tp * width
        slots = n_tp // 2 * GROUP
        rows = GROUP * length
        chans = in_x_w.shape[1] // 2
        units = ffn_down_w.shape[0] // 2
        shard = in_x_w.shape[0]
        bf16, f32 = jnp.bfloat16, jnp.float32
        shape = pltpu.VMEM
        normed_scratch = pltpu.VMEM((rows, features), bf16)

        def reduce_out(acts, weights, base):
            deep = weights[0].shape[0]
            send, keep = call(
                project_out_kernel,
                [shape((slots, length, width), bf16)] * 2,
                [acts, *weights],
                [pltpu.VMEM((deep, features), bf16)],
            )
            got = core_swap(send)
            own, *sent = call(
                join_kernel,
                [shape((length, width), f32)] + [shape((length, width), bf16)] * (slots - 1),
                [keep, got],
            )
            arrived = []
            for slot in range(1, slots):
                step, far = slot // GROUP * 2, slot % GROUP
                arrived.append(swap(sent[slot - 1], MATE * far, step))
            return call(finish_kernel, shape((length, width), bf16), [base, own, *arrived])

        in_parts = call(
            split_in_kernel,
            [shape((shard, 2 * chans), bf16)] * 2,
            [in_x_w, in_gate_w],
            space=pltpu.HBM,
        )
        shares = [shape((2 * units, shard), bf16), shape((units, shard), bf16)]
        ffn_parts = call(
            split_ffn_kernel, shares * 2, [ffn_gate_w.T, ffn_up_w.T, ffn_down_w], space=pltpu.HBM
        )
        pieces = whole_rows(tokens)
        in_w = gather(*in_parts)
        out_blocks = columns_of(out_w)
        up_w = gather(ffn_parts[0], ffn_parts[2])
        down_w = gather(ffn_parts[1], ffn_parts[3])
        mixer_out = call(
            functools.partial(mixer_kernel, len(pieces)),
            shape((rows, chans), bf16),
            [
                mix_gain[None],
                conv_taps,
                gate_x_blocks,
                gate_a_blocks,
                forget_rate[None],
                *pieces,
                *in_w,
            ],
            [normed_scratch, pltpu.VMEM((length + 8, chans), f32)],
        )
        mixed = whole_rows(mixer_out)
        after_mix = call(
            functools.partial(mix_project_kernel, len(pieces)),
            shape((rows, shard), bf16),
            [*mixed, *pieces, *out_blocks],
        )
        hidden, own = call(
            functools.partial(hidden_kernel, len(pieces)),
            [shape((rows, units), bf16), shape((length, width), bf16)],
            [ffn_gain[None], *whole_rows(after_mix), *up_w],
            [normed_scratch, pltpu.VMEM((length, features), bf16)],
        )
        return reduce_out(hidden, down_w, own)

    return on_device


def solution(mesh):
    n_fs, n_tp = mesh.shape["fs"], mesh.shape["tp"]
    placed = (
        P("fs", "tp"),
        P(),
        P("fs", "tp"),
        P("fs", "tp"),
        P(None, "tp"),
        P("tp", None, None),
        P("tp", None, None),
        P("tp"),
        P("tp", "fs"),
        P(),
        P("fs", "tp"),
        P("fs", "tp"),
        P("tp", "fs"),
    )
    made = sorted(turn_of(tp) ^ mate for tp in range(n_tp) for mate in (0, MATE))
    paired = made == list(range(n_fs))
    mapped = functools.partial(
        jax.shard_map, mesh=mesh, in_specs=placed, out_specs=P("fs", "tp"), check_vma=False
    )
    if paired:
        return mapped(paired_layer(n_fs, n_tp))
    return mapped(gathered_layer)
```

```python
import functools

import jax
import jax.numpy as jnp
from jax import lax
from jax.experimental import pallas as pl
from jax.experimental.pallas import tpu as pltpu
from jax.sharding import PartitionSpec as P

epsilon = 1e-06
gate_power = 8.0


def dot(left, right):
    return jnp.dot(left, right, preferred_element_type=jnp.float32)


def rms_norm(values, gain):
    wide = values.astype(jnp.float32)
    mean_square = jnp.mean(wide * wide, axis=-1, keepdims=True)
    return (wide * lax.rsqrt(mean_square + epsilon) * gain).astype(jnp.bfloat16)


def full_rows(shard):
    return lax.all_gather(shard, "tp", axis=1, tiled=True)


def project_out(acts, weight):
    partial_terms = dot(acts, lax.all_gather(weight, "fs", axis=1, tiled=True))
    return lax.psum_scatter(
        partial_terms.astype(jnp.bfloat16), "tp", scatter_dimension=1, tiled=True
    ).astype(jnp.float32)


def combine(earlier, later):
    return (earlier[0] * later[0], later[0] * earlier[1] + later[1])


def gathered_layer(
    tokens,
    mix_gain,
    in_x_w,
    in_gate_w,
    conv_taps,
    gate_x_blocks,
    gate_a_blocks,
    forget_rate,
    out_w,
    ffn_gain,
    ffn_gate_w,
    ffn_up_w,
    ffn_down_w,
):
    normed = rms_norm(full_rows(tokens), mix_gain)
    length = normed.shape[0]
    chan_width = in_x_w.shape[1]
    branch_in = dot(normed, lax.all_gather(in_x_w, "fs", axis=0, tiled=True))
    branch_gate = dot(normed, lax.all_gather(in_gate_w, "fs", axis=0, tiled=True))
    tap_count = conv_taps.shape[0]
    padded = jnp.pad(branch_in, ((tap_count - 1, 0), (0, 0)))
    conv_sum = padded[0:length] * conv_taps[0]
    for index in range(1, tap_count):
        conv_sum = conv_sum + padded[index : index + length] * conv_taps[index]
    conv_out = conv_sum.astype(jnp.bfloat16)
    blocks, block_dim = gate_x_blocks.shape[:2]
    grouped = conv_out.reshape(length, blocks, block_dim)

    def gate(maps):
        mapped = jnp.einsum("tbi,bij->tbj", grouped, maps, preferred_element_type=jnp.float32)
        return jax.nn.sigmoid(mapped.reshape(length, chan_width))

    log_decay = -gate_power * gate(gate_a_blocks) * forget_rate
    scale = jnp.sqrt(-jnp.expm1(2.0 * log_decay))
    scale = jnp.where((jnp.arange(length) == 0)[:, None], 1.0, scale)
    driven = conv_out.astype(jnp.float32) * gate(gate_x_blocks) * scale
    _, state = lax.associative_scan(combine, (jnp.exp(log_decay), driven), axis=0)
    mixer_out = (state * jax.nn.gelu(branch_gate)).astype(jnp.bfloat16)
    after_mix = (tokens.astype(jnp.float32) + project_out(mixer_out, out_w)).astype(jnp.bfloat16)
    normed_ffn = rms_norm(full_rows(after_mix), ffn_gain)
    gate_val = dot(normed_ffn, lax.all_gather(ffn_gate_w, "fs", axis=0, tiled=True))
    up_val = dot(normed_ffn, lax.all_gather(ffn_up_w, "fs", axis=0, tiled=True))
    hidden = (jax.nn.silu(gate_val) * up_val).astype(jnp.bfloat16)
    return (after_mix.astype(jnp.float32) + project_out(hidden, ffn_down_w)).astype(jnp.bfloat16)


MATE = 2
GROUP = 2
KERNEL_BYTES = 16 << 20


def side_of(fs):
    return lax.rem(lax.div(fs, MATE), 2)


def block_of(fs, entry, count):
    back = ((fs >> 1) - entry // 2) & (count // 2 - 1)
    return back * 2 + ((fs & 1) ^ (entry & 1))


def at(index, size):
    return pl.ds(pl.multiple_of(index * size, size), size)


def call(kernel, outs, args, scratch=(), space=pltpu.VMEM):
    spec = pl.BlockSpec(memory_space=pltpu.VMEM)
    return pl.pallas_call(
        kernel,
        out_shape=outs,
        in_specs=[spec] * len(args),
        out_specs=jax.tree.map(lambda _: spec, outs),
        scratch_shapes=list(scratch),
        compiler_params=pltpu.CompilerParams(vmem_limit_bytes=KERNEL_BYTES),
    )(*[pltpu.with_memory_space_constraint(arg, space) for arg in args])


def split_mix_kernel(x_ref, gate_ref, out_ref, *rest):
    count = (len(rest) - 2) // 2
    small, (mine_ref, other_ref), placed = rest[:count], rest[count : count + 2], rest[count + 2 :]
    for source, target in zip(small, placed):
        target[...] = source[...]
    side = side_of(lax.axis_index("fs"))
    depth, width = x_ref.shape
    half = width // 2
    for target, which in ((mine_ref, side), (other_ref, 1 - side)):
        target[:depth, :half] = x_ref[:, at(which, half)]
        target[:depth, half:] = gate_ref[:, at(which, half)]
        target[depth:] = out_ref[at(which, out_ref.shape[0] // 2), :]


def split_ffn_kernel(gate_ref, up_ref, down_ref, *results):
    side = side_of(lax.axis_index("fs"))
    half = gate_ref.shape[0] // 2
    for turn, which in enumerate((side, 1 - side)):
        up_part, down_part = results[2 * turn : 2 * turn + 2]
        up_part[:half] = gate_ref[at(which, half), :]
        up_part[half:] = up_ref[at(which, half), :]
        down_part[...] = down_ref[at(which, half), :]


def normalize(tp, row_refs, gain_ref, normed_ref):
    length, width = row_refs[0].shape
    slots = len(row_refs) // 2
    features = slots // GROUP * 2 * width
    for far in range(GROUP):
        pieces = []
        squares = 0.0
        for pair in range(slots // GROUP):
            for odd in range(2):
                wide = row_refs[odd * slots + pair * GROUP + far][...].astype(jnp.float32)
                squares = squares + jnp.sum(wide * wide, axis=1, keepdims=True)
                pieces.append((2 * pair + odd, wide))
        norm = lax.rsqrt(squares / features + epsilon)
        for step, wide in pieces:
            lanes = at(tp ^ step, width)
            scaled = wide * norm * gain_ref[:, lanes]
            normed_ref[far * length : (far + 1) * length, lanes] = scaled.astype(jnp.bfloat16)


def minus_expm1(value):
    series = 1.0 / 5040.0
    for factor in (720.0, 120.0, 24.0, 6.0, 2.0, 1.0):
        series = series * value + 1.0 / factor
    return jnp.where(value > -0.25, -value * series, 1.0 - jnp.exp(value))


def mixer_kernel(
    pieces, gain_ref, taps_ref, x_maps_ref, a_maps_ref, rate_ref, *rest
):
    row_refs, weights = rest[:pieces], rest[pieces:-3]
    out_ref, normed_ref, padded_ref = rest[-3:]
    fs = lax.axis_index("fs")
    tp = lax.axis_index("tp")
    side = side_of(fs)
    length = row_refs[0].shape[0]
    normalize(tp, row_refs, gain_ref, normed_ref)
    depth = normed_ref.shape[1] // len(weights)
    branches = dot(normed_ref[:, at(fs, depth)], weights[0][:depth])
    for step in range(1, len(weights)):
        lanes = at(block_of(fs, step, len(weights)), depth)
        branches = branches + dot(normed_ref[:, lanes], weights[step][:depth])
    chans = out_ref.shape[1]
    tap_count = taps_ref.shape[0]
    taps = taps_ref[:, at(side, chans)]
    rate = rate_ref[:, at(side, chans)]
    maps = x_maps_ref.shape[0] // 2
    size = x_maps_ref.shape[1]
    lead = padded_ref.shape[0] - length
    row = lax.broadcasted_iota(jnp.int32, (length, chans), 0)
    padded_ref[:lead] = jnp.zeros((lead, chans), jnp.float32)
    for far in range(GROUP):
        rows = slice(far * length, (far + 1) * length)
        padded_ref[lead:] = branches[rows, :chans]
        first = lead - tap_count + 1
        conv_sum = padded_ref[first : first + length] * taps[0:1]
        for index in range(1, tap_count):
            start = first + index
            conv_sum = conv_sum + padded_ref[start : start + length] * taps[index : index + 1]
        conv_out = conv_sum.astype(jnp.bfloat16)

        def gate(maps_ref):
            parts = [
                dot(conv_out[:, i * size : (i + 1) * size], maps_ref[side * maps + i])
                for i in range(maps)
            ]
            return jax.nn.sigmoid(jnp.concatenate(parts, axis=1) if maps > 1 else parts[0])

        log_decay = -gate_power * gate(a_maps_ref) * rate
        decay = jnp.exp(log_decay)
        scale = jnp.where(row == 0, 1.0, jnp.sqrt(minus_expm1(2.0 * log_decay)))
        state = conv_out.astype(jnp.float32) * gate(x_maps_ref) * scale
        reach = 1
        while reach < length:
            begun = row >= reach
            state = state + decay * jnp.where(begun, pltpu.roll(state, reach, 0), 0.0)
            decay = decay * jnp.where(begun, pltpu.roll(decay, reach, 0), 1.0)
            reach *= 2
        out_ref[rows, :] = (state * jax.nn.gelu(branches[rows, chans:])).astype(jnp.bfloat16)


def hidden_kernel(pieces, gain_ref, *rest):
    row_refs, weights = rest[:pieces], rest[pieces:-2]
    out_ref, normed_ref = rest[-2:]
    fs = lax.axis_index("fs")
    normalize(lax.axis_index("tp"), row_refs, gain_ref, normed_ref)
    units = out_ref.shape[1]
    depth = weights[0].shape[1]

    def project(first):
        total = None
        for step, weight in enumerate(weights):
            part = lax.dot_general(
                normed_ref[:, at(block_of(fs, step, len(weights)), depth)],
                weight[first : first + units, :],
                (((1,), (1,)), ((), ())),
                preferred_element_type=jnp.float32,
            )
            total = part if total is None else total + part
        return total

    out_ref[...] = (jax.nn.silu(project(0)) * project(units)).astype(jnp.bfloat16)


def project_out_kernel(first_step, acts_ref, *rest):
    *weights, send_ref, keep_ref, whole_ref = rest
    fs = lax.axis_index("fs")
    tp = lax.axis_index("tp")
    _, length, width = keep_ref.shape
    columns = weights[0].shape[1]
    for step, weight in enumerate(weights):
        first = weight.shape[0] - whole_ref.shape[0]
        whole_ref[:, at(block_of(fs, step, len(weights)), columns)] = weight[first:]
    for step, target in ((first_step + 1, send_ref), (first_step, keep_ref)):
        part = dot(acts_ref[...], whole_ref[:, at(tp ^ step, width)]).astype(jnp.bfloat16)
        for far in range(GROUP):
            target[far] = part[far * length : (far + 1) * length]


def join_kernel(keep_ref, got_ref, *outs):
    for far, out in enumerate(outs):
        total = keep_ref[far].astype(jnp.float32) + got_ref[far].astype(jnp.float32)
        out[...] = total.astype(out.dtype)


def finish_kernel(base_ref, *rest):
    *parts, out_ref = rest
    total = parts[0][...].astype(jnp.float32)
    for part in parts[1:]:
        total = total + part[...].astype(jnp.float32)
    out_ref[...] = (base_ref[...].astype(jnp.float32) + total).astype(jnp.bfloat16)


def paired_layer(n_fs, n_tp):
    def fs_swap(values, mask):
        return lax.ppermute(values, "fs", [(j, j ^ mask) for j in range(n_fs)])

    def core_swap(values):
        return lax.ppermute(values, "tp", [(j, j ^ 1) for j in range(n_tp)])

    def swap(values, fs_mask, tp_mask):
        pairs = [
            (a * n_tp + b, (a ^ fs_mask) * n_tp + (b ^ tp_mask))
            for a in range(n_fs)
            for b in range(n_tp)
        ]
        return lax.ppermute(values, ("fs", "tp"), pairs)

    def gather(mine, other):
        got = []
        for back in range(n_fs // 2):
            piece = mine
            if back:
                pairs = [(a, (a + 2 * back) % n_fs) for a in range(n_fs)]
                piece = lax.ppermute(other if back % 2 else mine, "fs", pairs)
            got += [piece, fs_swap(piece, 1)]
        return got

    def whole_rows(own):
        near = [own, swap(own, MATE, 0)]
        for step in range(2, n_tp, 2):
            near += [swap(piece, 0, step) for piece in near[:GROUP]]
        across = [core_swap(piece) for piece in near]
        return near + across

    def on_device(
        tokens,
        mix_gain,
        in_x_w,
        in_gate_w,
        conv_taps,
        gate_x_blocks,
        gate_a_blocks,
        forget_rate,
        out_w,
        ffn_gain,
        ffn_gate_w,
        ffn_up_w,
        ffn_down_w,
    ):
        length, width = tokens.shape
        features = n_tp * width
        rows = GROUP * length
        chans = in_x_w.shape[1] // 2
        units = ffn_down_w.shape[0] // 2
        shard = in_x_w.shape[0]
        bf16, f32 = jnp.bfloat16, jnp.float32
        shape = pltpu.VMEM
        normed_scratch = pltpu.VMEM((rows, features), bf16)

        def reduce_out(acts, weights, base, last):
            deep = acts.shape[1]
            arrived = []
            for step in range(n_tp - 2, -1, -2):
                send, keep = call(
                    functools.partial(project_out_kernel, step),
                    [shape((GROUP, length, width), bf16)] * 2,
                    [acts, *weights],
                    [pltpu.VMEM((deep, features), bf16)],
                )
                parts = call(
                    join_kernel,
                    [shape((length, width), bf16 if step + far else f32) for far in range(GROUP)],
                    [keep, core_swap(send)],
                )
                for far, part in enumerate(parts):
                    moved = swap(part, MATE * far, step) if step + far else part
                    arrived.append(moved)
            return call(finish_kernel, last((length, width), bf16), [base, *arrived])

        small = [mix_gain[None], conv_taps, gate_x_blocks, gate_a_blocks, forget_rate[None]]
        small += [ffn_gain[None], tokens]
        *mix_parts, mix_gain, conv_taps, gate_x_blocks, gate_a_blocks, forget_rate, ffn_gain, base = call(
            split_mix_kernel,
            [shape((shard + chans, 2 * chans), bf16)] * 2 + [shape(x.shape, x.dtype) for x in small],
            [in_x_w, in_gate_w, out_w, *small],
            space=pltpu.HBM,
        )
        shares = [shape((2 * units, shard), bf16), shape((units, shard), bf16)]
        ffn_parts = call(
            split_ffn_kernel, shares * 2, [ffn_gate_w.T, ffn_up_w.T, ffn_down_w], space=pltpu.HBM
        )
        pieces = whole_rows(tokens)
        pieces[0] = base
        mix_w = gather(*mix_parts)
        up_w = gather(ffn_parts[0], ffn_parts[2])
        down_w = gather(ffn_parts[1], ffn_parts[3])
        mixer_out = call(
            functools.partial(mixer_kernel, len(pieces)),
            shape((rows, chans), bf16),
            [
                mix_gain,
                conv_taps,
                gate_x_blocks,
                gate_a_blocks,
                forget_rate,
                *pieces,
                *mix_w,
            ],
            [normed_scratch, pltpu.VMEM((length + 8, chans), f32)],
        )
        after_mix = reduce_out(mixer_out, mix_w, base, shape)
        pieces = whole_rows(after_mix)
        hidden = call(
            functools.partial(hidden_kernel, len(pieces)),
            shape((rows, units), bf16),
            [ffn_gain, *pieces, *up_w],
            [normed_scratch],
        )
        return reduce_out(hidden, down_w, after_mix, jax.ShapeDtypeStruct)

    return on_device


def solution(mesh):
    n_fs, n_tp = mesh.shape["fs"], mesh.shape["tp"]
    placed = (
        P("fs", "tp"),
        P(),
        P("fs", "tp"),
        P("fs", "tp"),
        P(None, "tp"),
        P("tp", None, None),
        P("tp", None, None),
        P("tp"),
        P("tp", "fs"),
        P(),
        P("fs", "tp"),
        P("fs", "tp"),
        P("tp", "fs"),
    )
    paired = n_fs == GROUP * n_tp and n_tp % 2 == 0 and 2 * MATE < n_fs
    mapped = functools.partial(
        jax.shard_map, mesh=mesh, in_specs=placed, out_specs=P("fs", "tp"), check_vma=False
    )
    if paired:
        return mapped(paired_layer(n_fs, n_tp))
    return mapped(gathered_layer)
```

```python
import functools

import jax
import jax.numpy as jnp
from jax import lax
from jax.experimental import pallas as pl
from jax.experimental.pallas import tpu as pltpu
from jax.sharding import PartitionSpec as P

epsilon = 1e-06
gate_power = 8.0


def dot(left, right):
    return jnp.dot(left, right, preferred_element_type=jnp.float32)


def rms_norm(values, gain):
    wide = values.astype(jnp.float32)
    mean_square = jnp.mean(wide * wide, axis=-1, keepdims=True)
    return (wide * lax.rsqrt(mean_square + epsilon) * gain).astype(jnp.bfloat16)


def full_rows(shard):
    return lax.all_gather(shard, "tp", axis=1, tiled=True)


def project_out(acts, weight):
    partial_terms = dot(acts, lax.all_gather(weight, "fs", axis=1, tiled=True))
    return lax.psum_scatter(
        partial_terms.astype(jnp.bfloat16), "tp", scatter_dimension=1, tiled=True
    ).astype(jnp.float32)


def combine(earlier, later):
    return (earlier[0] * later[0], later[0] * earlier[1] + later[1])


def gathered_layer(
    tokens,
    mix_gain,
    in_x_w,
    in_gate_w,
    conv_taps,
    gate_x_blocks,
    gate_a_blocks,
    forget_rate,
    out_w,
    ffn_gain,
    ffn_gate_w,
    ffn_up_w,
    ffn_down_w,
):
    normed = rms_norm(full_rows(tokens), mix_gain)
    length = normed.shape[0]
    chan_width = in_x_w.shape[1]
    branch_in = dot(normed, lax.all_gather(in_x_w, "fs", axis=0, tiled=True))
    branch_gate = dot(normed, lax.all_gather(in_gate_w, "fs", axis=0, tiled=True))
    tap_count = conv_taps.shape[0]
    padded = jnp.pad(branch_in, ((tap_count - 1, 0), (0, 0)))
    conv_sum = padded[0:length] * conv_taps[0]
    for index in range(1, tap_count):
        conv_sum = conv_sum + padded[index : index + length] * conv_taps[index]
    conv_out = conv_sum.astype(jnp.bfloat16)
    blocks, block_dim = gate_x_blocks.shape[:2]
    grouped = conv_out.reshape(length, blocks, block_dim)

    def gate(maps):
        mapped = jnp.einsum("tbi,bij->tbj", grouped, maps, preferred_element_type=jnp.float32)
        return jax.nn.sigmoid(mapped.reshape(length, chan_width))

    log_decay = -gate_power * gate(gate_a_blocks) * forget_rate
    scale = jnp.sqrt(-jnp.expm1(2.0 * log_decay))
    scale = jnp.where((jnp.arange(length) == 0)[:, None], 1.0, scale)
    driven = conv_out.astype(jnp.float32) * gate(gate_x_blocks) * scale
    _, state = lax.associative_scan(combine, (jnp.exp(log_decay), driven), axis=0)
    mixer_out = (state * jax.nn.gelu(branch_gate)).astype(jnp.bfloat16)
    after_mix = (tokens.astype(jnp.float32) + project_out(mixer_out, out_w)).astype(jnp.bfloat16)
    normed_ffn = rms_norm(full_rows(after_mix), ffn_gain)
    gate_val = dot(normed_ffn, lax.all_gather(ffn_gate_w, "fs", axis=0, tiled=True))
    up_val = dot(normed_ffn, lax.all_gather(ffn_up_w, "fs", axis=0, tiled=True))
    hidden = (jax.nn.silu(gate_val) * up_val).astype(jnp.bfloat16)
    return (after_mix.astype(jnp.float32) + project_out(hidden, ffn_down_w)).astype(jnp.bfloat16)


MATE = 2
GROUP = 2
KERNEL_BYTES = 16 << 20


def side_of(fs):
    return lax.rem(lax.div(fs, MATE), 2)


def block_of(fs, entry, count):
    back = ((fs >> 1) - entry // 2) & (count // 2 - 1)
    return back * 2 + ((fs & 1) ^ (entry & 1))


def at(index, size):
    return pl.ds(pl.multiple_of(index * size, size), size)


def call(kernel, outs, args, scratch=(), space=pltpu.VMEM):
    spec = pl.BlockSpec(memory_space=pltpu.VMEM)
    return pl.pallas_call(
        kernel,
        out_shape=outs,
        in_specs=[spec] * len(args),
        out_specs=jax.tree.map(lambda _: spec, outs),
        scratch_shapes=list(scratch),
        compiler_params=pltpu.CompilerParams(vmem_limit_bytes=KERNEL_BYTES),
    )(*[pltpu.with_memory_space_constraint(arg, space) for arg in args])


def split_mix_kernel(x_ref, gate_ref, out_ref, *rest):
    count = (len(rest) - 2) // 2
    small, (mine_ref, other_ref), placed = rest[:count], rest[count : count + 2], rest[count + 2 :]
    for source, target in zip(small, placed):
        target[...] = source[...]
    side = side_of(lax.axis_index("fs"))
    depth, width = x_ref.shape
    half = width // 2
    for target, which in ((mine_ref, side), (other_ref, 1 - side)):
        target[:depth, :half] = x_ref[:, at(which, half)]
        target[:depth, half:] = gate_ref[:, at(which, half)]
        target[depth:] = out_ref[at(which, out_ref.shape[0] // 2), :]


def split_ffn_kernel(gate_ref, up_ref, down_ref, *results):
    side = side_of(lax.axis_index("fs"))
    half = gate_ref.shape[0] // 2
    for turn, which in enumerate((side, 1 - side)):
        up_part, down_part = results[2 * turn : 2 * turn + 2]
        up_part[:half] = gate_ref[at(which, half), :]
        up_part[half:] = up_ref[at(which, half), :]
        down_part[...] = down_ref[at(which, half), :]


def normalize(tp, row_refs, gain_ref, normed_ref):
    length, width = row_refs[0].shape
    slots = len(row_refs) // 2
    features = slots // GROUP * 2 * width
    for far in range(GROUP):
        pieces = []
        squares = 0.0
        for pair in range(slots // GROUP):
            for odd in range(2):
                wide = row_refs[odd * slots + pair * GROUP + far][...].astype(jnp.float32)
                squares = squares + jnp.sum(wide * wide, axis=1, keepdims=True)
                pieces.append((2 * pair + odd, wide))
        norm = lax.rsqrt(squares / features + epsilon)
        for step, wide in pieces:
            lanes = at(tp ^ step, width)
            scaled = wide * norm * gain_ref[:, lanes]
            normed_ref[far * length : (far + 1) * length, lanes] = scaled.astype(jnp.bfloat16)


def minus_expm1(value):
    series = 1.0 / 5040.0
    for factor in (720.0, 120.0, 24.0, 6.0, 2.0, 1.0):
        series = series * value + 1.0 / factor
    return jnp.where(value > -0.25, -value * series, 1.0 - jnp.exp(value))


def mixer_kernel(
    pieces, gain_ref, taps_ref, x_maps_ref, a_maps_ref, rate_ref, *rest
):
    row_refs, weights = rest[:pieces], rest[pieces:-3]
    out_ref, normed_ref, padded_ref = rest[-3:]
    fs = lax.axis_index("fs")
    tp = lax.axis_index("tp")
    side = side_of(fs)
    length = row_refs[0].shape[0]
    normalize(tp, row_refs, gain_ref, normed_ref)
    depth = normed_ref.shape[1] // len(weights)
    branches = dot(normed_ref[:, at(fs, depth)], weights[0][:depth])
    for step in range(1, len(weights)):
        lanes = at(block_of(fs, step, len(weights)), depth)
        branches = branches + dot(normed_ref[:, lanes], weights[step][:depth])
    chans = out_ref.shape[1]
    tap_count = taps_ref.shape[0]
    taps = taps_ref[:, at(side, chans)]
    rate = rate_ref[:, at(side, chans)]
    maps = x_maps_ref.shape[0] // 2
    size = x_maps_ref.shape[1]
    lead = padded_ref.shape[0] - length
    row = lax.broadcasted_iota(jnp.int32, (length, chans), 0)
    padded_ref[:lead] = jnp.zeros((lead, chans), jnp.float32)
    for far in range(GROUP):
        rows = slice(far * length, (far + 1) * length)
        padded_ref[lead:] = branches[rows, :chans]
        first = lead - tap_count + 1
        conv_sum = padded_ref[first : first + length] * taps[0:1]
        for index in range(1, tap_count):
            start = first + index
            conv_sum = conv_sum + padded_ref[start : start + length] * taps[index : index + 1]
        conv_out = conv_sum.astype(jnp.bfloat16)

        def gate(maps_ref):
            parts = [
                dot(conv_out[:, i * size : (i + 1) * size], maps_ref[side * maps + i])
                for i in range(maps)
            ]
            return jax.nn.sigmoid(jnp.concatenate(parts, axis=1) if maps > 1 else parts[0])

        log_decay = -gate_power * gate(a_maps_ref) * rate
        decay = jnp.exp(log_decay)
        scale = jnp.where(row == 0, 1.0, jnp.sqrt(minus_expm1(2.0 * log_decay)))
        state = conv_out.astype(jnp.float32) * gate(x_maps_ref) * scale
        reach = 1
        while reach < length:
            begun = row >= reach
            state = state + decay * jnp.where(begun, pltpu.roll(state, reach, 0), 0.0)
            decay = decay * jnp.where(begun, pltpu.roll(decay, reach, 0), 1.0)
            reach *= 2
        out_ref[rows, :] = (state * jax.nn.gelu(branches[rows, chans:])).astype(jnp.bfloat16)


def project_rows(normed_ref, weights, entries, count, first, units):
    total = None
    for entry, weight in zip(entries, weights):
        depth = weight.shape[1]
        part = lax.dot_general(
            normed_ref[:, at(block_of(lax.axis_index("fs"), entry, count), depth)],
            weight[first : first + units, :],
            (((1,), (1,)), ((), ())),
            preferred_element_type=jnp.float32,
        )
        total = part if total is None else total + part
    return total


def early_kernel(pieces, entries, count, gain_ref, *rest):
    row_refs, weights = rest[:pieces], rest[pieces:-3]
    gate_ref, up_ref, normed_ref = rest[-3:]
    normalize(lax.axis_index("tp"), row_refs, gain_ref, normed_ref)
    units = gate_ref.shape[1]
    gate_ref[...] = project_rows(normed_ref, weights, entries, count, 0, units)
    up_ref[...] = project_rows(normed_ref, weights, entries, count, units, units)


def hidden_kernel(entries, count, gate_ref, up_ref, normed_ref, *rest):
    *weights, out_ref = rest
    units = out_ref.shape[1]
    gate = gate_ref[...] + project_rows(normed_ref, weights, entries, count, 0, units)
    up = up_ref[...] + project_rows(normed_ref, weights, entries, count, units, units)
    out_ref[...] = (jax.nn.silu(gate) * up).astype(jnp.bfloat16)


def project_out_kernel(first_step, acts_ref, *rest):
    *weights, send_ref, keep_ref, whole_ref = rest
    fs = lax.axis_index("fs")
    tp = lax.axis_index("tp")
    _, length, width = keep_ref.shape
    columns = weights[0].shape[1]
    for step, weight in enumerate(weights):
        first = weight.shape[0] - whole_ref.shape[0]
        whole_ref[:, at(block_of(fs, step, len(weights)), columns)] = weight[first:]
    for step, target in ((first_step + 1, send_ref), (first_step, keep_ref)):
        part = dot(acts_ref[...], whole_ref[:, at(tp ^ step, width)]).astype(jnp.bfloat16)
        for far in range(GROUP):
            target[far] = part[far * length : (far + 1) * length]


def join_kernel(keep_ref, got_ref, *outs):
    for far, out in enumerate(outs):
        total = keep_ref[far].astype(jnp.float32) + got_ref[far].astype(jnp.float32)
        out[...] = total.astype(out.dtype)


def gather_sum_kernel(*refs):
    *parts, out_ref = refs
    for far in range(GROUP):
        total = parts[far][...].astype(jnp.float32)
        for part in parts[GROUP + far :: GROUP]:
            total = total + part[...].astype(jnp.float32)
        out_ref[far] = total.astype(jnp.bfloat16)


def add_pair_kernel(own_ref, mate_ref, made_ref, got_ref, *outs):
    for far, (base_ref, out) in enumerate(zip((own_ref, mate_ref), outs)):
        total = made_ref[far].astype(jnp.float32) + got_ref[far ^ 1].astype(jnp.float32)
        out[...] = (base_ref[...].astype(jnp.float32) + total).astype(jnp.bfloat16)


def finish_kernel(base_ref, *rest):
    *parts, out_ref = rest
    total = parts[0][...].astype(jnp.float32)
    for part in parts[1:]:
        total = total + part[...].astype(jnp.float32)
    out_ref[...] = (base_ref[...].astype(jnp.float32) + total).astype(jnp.bfloat16)


def paired_layer(n_fs, n_tp):
    def fs_swap(values, mask):
        return lax.ppermute(values, "fs", [(j, j ^ mask) for j in range(n_fs)])

    def core_swap(values):
        return lax.ppermute(values, "tp", [(j, j ^ 1) for j in range(n_tp)])

    def swap(values, fs_mask, tp_mask):
        pairs = [
            (a * n_tp + b, (a ^ fs_mask) * n_tp + (b ^ tp_mask))
            for a in range(n_fs)
            for b in range(n_tp)
        ]
        return lax.ppermute(values, ("fs", "tp"), pairs)

    def gather(mine, other):
        got = []
        for back in range(n_fs // 2):
            piece = mine
            if back:
                pairs = [(a, (a + 2 * back) % n_fs) for a in range(n_fs)]
                piece = lax.ppermute(other if back % 2 else mine, "fs", pairs)
            got += [piece, fs_swap(piece, 1)]
        return got

    def whole_rows(near):
        near = list(near)
        for step in range(2, n_tp, 2):
            near += [swap(piece, 0, step) for piece in near[:GROUP]]
        return near + [core_swap(piece) for piece in near]

    def on_device(
        tokens,
        mix_gain,
        in_x_w,
        in_gate_w,
        conv_taps,
        gate_x_blocks,
        gate_a_blocks,
        forget_rate,
        out_w,
        ffn_gain,
        ffn_gate_w,
        ffn_up_w,
        ffn_down_w,
    ):
        length, width = tokens.shape
        features = n_tp * width
        rows = GROUP * length
        chans = in_x_w.shape[1] // 2
        units = ffn_down_w.shape[0] // 2
        shard = in_x_w.shape[0]
        bf16, f32 = jnp.bfloat16, jnp.float32
        shape = pltpu.VMEM
        normed_scratch = pltpu.VMEM((rows, features), bf16)

        def core_sums(acts, weights, kinds):
            deep = acts.shape[1]
            for step in range(n_tp - 2, -1, -2):
                send, keep = call(
                    functools.partial(project_out_kernel, step),
                    [shape((GROUP, length, width), bf16)] * 2,
                    [acts, *weights],
                    [pltpu.VMEM((deep, features), bf16)],
                )
                parts = call(
                    join_kernel,
                    [shape((length, width), bf16 if step else kind) for kind in kinds],
                    [keep, core_swap(send)],
                )
                yield step, parts

        def reduce_both(acts, weights, bases):
            found = []
            for step, parts in core_sums(acts, weights, (f32, f32)):
                for part in parts:
                    found.append(swap(part, 0, step) if step else part)
            made = call(gather_sum_kernel, shape((GROUP, length, width), bf16), found)
            return call(
                add_pair_kernel,
                [shape((length, width), bf16)] * GROUP,
                [*bases, made, swap(made, MATE, 0)],
            )

        def reduce_own(acts, weights, base):
            found = []
            for step, parts in core_sums(acts, weights, (f32, bf16)):
                for far, part in enumerate(parts):
                    moved = step + far
                    found.append(swap(part, MATE * far, step) if moved else part)
            return call(finish_kernel, jax.ShapeDtypeStruct((length, width), bf16), [base, *found])

        small = [mix_gain[None], conv_taps, gate_x_blocks, gate_a_blocks, forget_rate[None]]
        small += [ffn_gain[None], tokens]
        *mix_parts, mix_gain, conv_taps, gate_x_blocks, gate_a_blocks, forget_rate, ffn_gain, base = call(
            split_mix_kernel,
            [shape((shard + chans, 2 * chans), bf16)] * 2 + [shape(x.shape, x.dtype) for x in small],
            [in_x_w, in_gate_w, out_w, *small],
            space=pltpu.HBM,
        )
        shares = [shape((2 * units, shard), bf16), shape((units, shard), bf16)]
        ffn_parts = call(
            split_ffn_kernel, shares * 2, [ffn_gate_w.T, ffn_up_w.T, ffn_down_w], space=pltpu.HBM
        )
        bases = [base, swap(tokens, MATE, 0)]
        pieces = whole_rows(bases)
        mix_w = gather(*mix_parts)
        up_w = gather(ffn_parts[0], ffn_parts[2])
        down_w = gather(ffn_parts[1], ffn_parts[3])
        mixer_out = call(
            functools.partial(mixer_kernel, len(pieces)),
            shape((rows, chans), bf16),
            [
                mix_gain,
                conv_taps,
                gate_x_blocks,
                gate_a_blocks,
                forget_rate,
                *pieces,
                *mix_w,
            ],
            [normed_scratch, pltpu.VMEM((length + 8, chans), f32)],
        )
        after_mix = reduce_both(mixer_out, mix_w, bases)
        pieces = whole_rows(after_mix)
        late = [entry for entry in range(n_fs) if entry // 2 == n_fs // 4]
        early = [entry for entry in range(n_fs) if entry not in late]
        sums = call(
            functools.partial(early_kernel, len(pieces), early, n_fs),
            [shape((rows, units), f32)] * 2 + [shape((rows, features), bf16)],
            [ffn_gain, *pieces, *[up_w[entry] for entry in early]],
        )
        hidden = call(
            functools.partial(hidden_kernel, late, n_fs),
            shape((rows, units), bf16),
            [*sums, *[up_w[entry] for entry in late]],
        )
        return reduce_own(hidden, down_w, after_mix[0])

    return on_device


def solution(mesh):
    n_fs, n_tp = mesh.shape["fs"], mesh.shape["tp"]
    placed = (
        P("fs", "tp"),
        P(),
        P("fs", "tp"),
        P("fs", "tp"),
        P(None, "tp"),
        P("tp", None, None),
        P("tp", None, None),
        P("tp"),
        P("tp", "fs"),
        P(),
        P("fs", "tp"),
        P("fs", "tp"),
        P("tp", "fs"),
    )
    paired = n_fs == GROUP * n_tp and n_tp % 2 == 0 and 2 * MATE < n_fs
    mapped = functools.partial(
        jax.shard_map, mesh=mesh, in_specs=placed, out_specs=P("fs", "tp"), check_vma=False
    )
    if paired:
        return mapped(paired_layer(n_fs, n_tp))
    return mapped(gathered_layer)
```
